32 devices in a mesh: sp: 4 (over y, x), tp: 8 (over z, core).
Axes of the slice: x: 2, y: 2, z: 4, core: 2. Of those that a mesh axis runs over, the one named last changes fastest.
Arguments:
- ask_preactivation_left: bfloat16 [2048, 2048], P('sp', 'tp'), may hold values from -6 to 6
- keep_preactivation_left: bfloat16 [2048, 2048], P('sp', 'tp'), may hold values from -6 to 6
- keep_bound_complement_left: float32 [2048], P('tp'), may hold values from 0 to 0.1
- ask_preactivation_right: bfloat16 [2048, 4096], P('sp', 'tp'), may hold values from -6 to 6
- keep_preactivation_right: bfloat16 [2048, 4096], P('sp', 'tp'), may hold values from -6 to 6
- keep_bound_complement_right: float32 [4096], P('tp'), may hold values from 0 to 0.1
- payload_entries: bfloat16 [2048, 2048], P('sp', 'tp'), may hold values from -6 to 6
- emission_switch_logits: bfloat16 [2048, 2048], P('sp', 'tp'), may hold values from -6 to 6
- added_log_keep_bias: float32 [2048, 32], P('sp', 'tp'), may hold values from -2.1 to 0
- lanewise_rescale: float32 [64], replicated, may hold values from 0.1 to 1.9
- emission_matrix_alpha: bfloat16 [1024, 2048], P('tp'), may hold values from -0.125 to 0.125
- emission_matrix_beta: bfloat16 [1024, 2048], P('tp'), may hold values from -0.125 to 0.125
- skip_stream: bfloat16 [2048, 2048], P(('sp', 'tp')), may hold values from -6 to 6
- postrecurrence_rescale: float32 [2048], replicated, may hold values from 0.1 to 1.9
- premixture_rescale: float32 [2048], replicated, may hold values from 0.1 to 1.9
- postmixture_rescale: float32 [2048], replicated, may hold values from 0.1 to 1.9
- dispatcher_columns: bfloat16 [2048, 8], P(None, 'sp'), may hold values from -0.125 to 0.125
- switch_matrix: bfloat16 [4, 2048, 4096], P('sp', None, 'tp'), may hold values from -0.125 to 0.125
- expansion_matrix: bfloat16 [4, 2048, 4096], P('sp', None, 'tp'), may hold values from -0.125 to 0.125
- contraction_matrix: bfloat16 [4, 4096, 2048], P('sp', 'tp'), may hold values from -0.125 to 0.125
- item_specialist_cluster: int32 [2048], P(('sp', 'tp')), may hold values from 0 to 3, as said below
Outputs:
- result: bfloat16 [2048, 2048], P(('sp', 'tp'))
The draws below stay inside these ranges and needn't reach their ends.
Inputs may be any that keep to these rules, and one draw needn't show every extreme that they name: `item_specialist_cluster`: in every aligned block of 64 tokens (the rows of one device) no group is named more than 18 times, and some group exactly 18 times.
All inputs are finite; a program needn't handle non-finite values.
Results may differ from the reference program's by a relative error of at most 0.023.
Values may be sent and summed in bfloat16 or wider, within the bound.
A program may use at most 64 MiB of HBM per device.

```python
import jax
import jax.numpy as jnp
from jax import lax

D = 2048
HEADS_IN_SET = 16
DKA = 128
DKB = 256
DV = 64
FF = 2048
EXP_GROUP = 2
TOK_DEV = 512
BLOCK_LENGTH = 512
SEQ_STEPS = 2048
ROWS_DEV = 64
GROUPS = 4
EXPERTS = 8
CAP = 18
N_TP = 8


def forget_draw(key, columns):
    noise_part = jnp.clip(jax.random.normal(jax.random.fold_in(key, 1), (SEQ_STEPS, columns), jnp.float32), -5.0, 5.0)
    block_shift = jax.random.uniform(jax.random.fold_in(key, 2), (SEQ_STEPS // TOK_DEV, 1, 1), jnp.float32, -1.0, 1.0)
    shifted = noise_part.reshape(SEQ_STEPS // TOK_DEV, TOK_DEV, columns) + block_shift
    return shifted.reshape(SEQ_STEPS, columns).astype(jnp.bfloat16)


def draw_keep_preactivation_left(key, part):
    return forget_draw(key, HEADS_IN_SET * DKA)


def draw_keep_preactivation_right(key, part):
    return forget_draw(key, HEADS_IN_SET * DKB)


def gap_draw(key, recurrent_state_width):
    fast_share = 0.5
    fast_head = jax.random.uniform(jax.random.fold_in(key, 21), (HEADS_IN_SET, 1), jnp.float32) < fast_share
    quick_gap = jnp.exp(jax.random.uniform(jax.random.fold_in(key, 22), (HEADS_IN_SET, recurrent_state_width), jnp.float32, jnp.log(0.04), jnp.log(0.1)))
    slow_gap = jnp.exp(jax.random.uniform(jax.random.fold_in(key, 23), (HEADS_IN_SET, recurrent_state_width), jnp.float32, jnp.log(0.3 / SEQ_STEPS), jnp.log(1.5 / SEQ_STEPS)))
    return jnp.where(fast_head, quick_gap, slow_gap).reshape(HEADS_IN_SET * recurrent_state_width)


def draw_keep_bound_complement_left(key, part):
    return gap_draw(key, DKA)


def draw_keep_bound_complement_right(key, part):
    return gap_draw(key, DKB)


def draw_added_log_keep_bias(key, part):
    spike_position = jax.random.randint(jax.random.fold_in(key, 31), (3, 2 * HEADS_IN_SET), 0, SEQ_STEPS)
    spike_strength = jax.random.uniform(jax.random.fold_in(key, 32), (3, 2 * HEADS_IN_SET), jnp.float32, jnp.log(0.5), jnp.log(0.8))
    sequence_positions = jnp.arange(SEQ_STEPS, dtype=jnp.int32)[:, None]
    spike_sum = jnp.zeros((SEQ_STEPS, 2 * HEADS_IN_SET), jnp.float32)
    for selected_group in range(3):
        spike_sum = spike_sum + jnp.where(sequence_positions == spike_position[selected_group][None, :], spike_strength[selected_group][None, :], 0.0)
    return spike_sum


def draw_item_specialist_cluster(key, part):
    block_total_count = SEQ_STEPS // ROWS_DEV
    others = GROUPS - 1
    spare_rows = ROWS_DEV - CAP
    base_load = spare_rows // others
    extra_rows = spare_rows - base_load * others
    move_limit = max(0, min(CAP - base_load - 1, base_load))
    hot_group = jax.random.randint(jax.random.fold_in(key, 11), (block_total_count, 1), 0, GROUPS)
    other_index = jnp.arange(others, dtype=jnp.int32)[None, :]
    shuffled = jnp.argsort(jax.random.randint(jax.random.fold_in(key, 12), (block_total_count, others), 0, 1 << 16) * others + other_index, axis=1)
    loads = base_load + (shuffled < extra_rows).astype(jnp.int32)
    pairs = others // 2
    if pairs > 0:
        moved = jax.random.randint(jax.random.fold_in(key, 13), (block_total_count, pairs), -move_limit, move_limit + 1)
        load_shift = jnp.stack([moved, -moved], axis=2).reshape(block_total_count, 2 * pairs)
        if others > 2 * pairs:
            load_shift = jnp.concatenate([load_shift, jnp.zeros((block_total_count, 1), jnp.int32)], axis=1)
        loads = loads + load_shift
    group_index = jnp.arange(GROUPS, dtype=jnp.int32)[None, :]
    source = jnp.clip(jnp.where(group_index < hot_group, group_index, group_index - 1), 0, others - 1)
    source = jnp.broadcast_to(source, (block_total_count, GROUPS))
    all_loads = jnp.where(group_index == hot_group, CAP, jnp.take_along_axis(loads, source, axis=1))
    load_ends = jnp.cumsum(all_loads, axis=1)
    sequence_positions = jnp.arange(ROWS_DEV, dtype=jnp.int32)[None, :, None]
    group_of = jnp.sum((load_ends[:, None, :] <= sequence_positions).astype(jnp.int32), axis=2)
    row_index = jnp.arange(ROWS_DEV, dtype=jnp.int32)[None, :]
    row_order = jnp.argsort(jax.random.randint(jax.random.fold_in(key, 14), (block_total_count, ROWS_DEV), 0, 1 << 16) * ROWS_DEV + row_index, axis=1)
    group_of = jnp.take_along_axis(group_of, row_order, axis=1)
    return group_of.reshape(SEQ_STEPS).astype(jnp.int32)


def steps_of(own_key, extent, split, smallest, high):
    loudness, own = 1.0, jax.random.fold_in(own_key, 6)
    for dim, shards_of in split:
        steps = jnp.exp(jax.random.uniform(jax.random.fold_in(own, dim), (shards_of,), jnp.float32, smallest / len(split), high / len(split)))
        loudness = loudness * jnp.repeat(steps, extent[dim] // shards_of).reshape([-1 if axis == dim else 1 for axis in range(len(extent))])
    return loudness


def gaussian(rng, extent, width, bound, split=(), kind=jnp.bfloat16):
    level = steps_of(rng, extent, split, -0.22, 0.18) if split else 1.0
    drawn = jax.random.normal(rng, extent, jnp.float32) * width * level
    return jnp.minimum(jnp.maximum(drawn, -bound), bound).astype(kind)


def setup_inputs(seed: int = 0) -> dict:
    key_list = jax.random.split(jax.random.key(seed), 22)
    return {
        "ask_preactivation_left": gaussian(key_list[0], (SEQ_STEPS, HEADS_IN_SET * DKA), 1.0, 6.0, ((0, 4), (1, 8))),
        "keep_preactivation_left": draw_keep_preactivation_left(jax.random.fold_in(key_list[21], 71), 0),
        "keep_bound_complement_left": draw_keep_bound_complement_left(jax.random.fold_in(key_list[21], 71), 0),
        "ask_preactivation_right": gaussian(key_list[3], (SEQ_STEPS, HEADS_IN_SET * DKB), 1.0, 6.0, ((0, 4), (1, 8))),
        "keep_preactivation_right": draw_keep_preactivation_right(jax.random.fold_in(key_list[21], 71), 0),
        "keep_bound_complement_right": draw_keep_bound_complement_right(jax.random.fold_in(key_list[21], 71), 0),
        "payload_entries": gaussian(key_list[6], (SEQ_STEPS, 2 * HEADS_IN_SET * DV), 1.0, 6.0, ((0, 4), (1, 8))),
        "emission_switch_logits": gaussian(key_list[7], (SEQ_STEPS, 2 * HEADS_IN_SET * DV), 1.0, 6.0, ((0, 4), (1, 8))),
        "added_log_keep_bias": draw_added_log_keep_bias(jax.random.fold_in(key_list[21], 71), 0),
        "lanewise_rescale": jnp.clip(1.0 + 0.18 * jax.random.normal(key_list[9], (DV,), jnp.float32), 0.1, 1.9),
        "emission_matrix_alpha": gaussian(key_list[10], (HEADS_IN_SET * DV, D), (2 * HEADS_IN_SET * DV) ** -0.5, 0.125, ((0, 8),)),
        "emission_matrix_beta": gaussian(key_list[11], (HEADS_IN_SET * DV, D), (2 * HEADS_IN_SET * DV) ** -0.5, 0.125, ((0, 8),)),
        "skip_stream": gaussian(key_list[12], (SEQ_STEPS, D), 1.0, 6.0, ((0, 32),)),
        "postrecurrence_rescale": jnp.clip(1.0 + 0.18 * jax.random.normal(key_list[13], (D,), jnp.float32), 0.1, 1.9),
        "premixture_rescale": jnp.clip(1.0 + 0.18 * jax.random.normal(key_list[14], (D,), jnp.float32), 0.1, 1.9),
        "postmixture_rescale": jnp.clip(1.0 + 0.18 * jax.random.normal(key_list[15], (D,), jnp.float32), 0.1, 1.9),
        "dispatcher_columns": gaussian(key_list[16], (D, EXPERTS), D ** -0.5, 0.125, ((1, 4),)),
        "switch_matrix": gaussian(key_list[17], (GROUPS, D, EXP_GROUP * FF), D ** -0.5, 0.125, ((0, 4), (2, 8))),
        "expansion_matrix": gaussian(key_list[18], (GROUPS, D, EXP_GROUP * FF), D ** -0.5, 0.125, ((0, 4), (2, 8))),
        "contraction_matrix": gaussian(key_list[19], (GROUPS, EXP_GROUP * FF, D), FF ** -0.5, 0.125, ((0, 4), (1, 8))),
        "item_specialist_cluster": draw_item_specialist_cluster(jax.random.fold_in(key_list[21], 71), 0),
    }


EPSILON = 1e-06
PRECISE = lax.Precision.HIGHEST

def rms_scale(features, gain):
    return features * lax.rsqrt(lax.optimization_barrier(jnp.mean(features * features, axis=-1, keepdims=True)) + EPSILON) * gain

def block_step(carry_state, inputs):
    queries, incoming_key_rows, value_row_block, inside = inputs
    length = queries.shape[0]
    causal = lax.broadcasted_iota(jnp.int32, (length, length), 0) >= lax.broadcasted_iota(jnp.int32, (length, length), 1)
    q_decayed = queries * jnp.exp(inside)
    k_grown = incoming_key_rows * jnp.exp(-inside)
    scores = jnp.einsum('thd,shd->hts', q_decayed, k_grown, precision=PRECISE)
    scores = jnp.where(causal[None], scores, jnp.zeros_like(scores))
    outputs = jnp.einsum('hts,shv->thv', scores, value_row_block, precision=PRECISE)
    outputs = outputs + jnp.einsum('thd,hdv->thv', q_decayed, carry_state, precision=PRECISE)
    last_decay = inside[-1]
    fresh_state = jnp.einsum('shd,shv->hdv', incoming_key_rows * jnp.exp(last_decay[None] - inside), value_row_block, precision=PRECISE)
    return (jnp.exp(last_decay)[:, :, None] * carry_state + fresh_state, outputs)

def head_outputs(call_arguments):
    query_vector, forget_gate, lower_margin, spike_value, value_row_block = call_arguments
    recurrent_state_width = query_vector.shape[1]
    block_total_count = SEQ_STEPS // BLOCK_LENGTH
    block_shape = (block_total_count, BLOCK_LENGTH, 1, recurrent_state_width)
    queries = jax.nn.silu(query_vector.astype(jnp.float32)).reshape(block_shape)
    incoming_key_rows = lower_margin * jax.nn.sigmoid(-forget_gate.astype(jnp.float32)).reshape(block_shape)
    logarithm_decay = jnp.log1p(-incoming_key_rows) + spike_value.reshape(block_total_count, BLOCK_LENGTH, 1, 1)
    inside = jnp.cumsum(logarithm_decay, axis=1)
    start_state = jnp.zeros((1, recurrent_state_width, DV), jnp.float32)
    final_state, outputs = lax.scan(block_step, start_state, (queries, incoming_key_rows, value_row_block.reshape(block_total_count, BLOCK_LENGTH, 1, DV), inside))
    return outputs.reshape(SEQ_STEPS, DV)

def partitioned_result_array(query_vector, forget_gate, lower_margin, spike_value, value_row_block):
    recurrent_state_width = query_vector.shape[1] // HEADS_IN_SET
    per_head_split = (query_vector.reshape(SEQ_STEPS, HEADS_IN_SET, recurrent_state_width).transpose(1, 0, 2), forget_gate.reshape(SEQ_STEPS, HEADS_IN_SET, recurrent_state_width).transpose(1, 0, 2), lower_margin.reshape(HEADS_IN_SET, recurrent_state_width), spike_value.T, value_row_block.transpose(1, 0, 2))
    outputs = lax.map(head_outputs, per_head_split)
    return outputs.transpose(1, 0, 2)

def head_rows(outputs, gate_rows, lanewise_rescale):
    scaled = rms_scale(outputs, lanewise_rescale) * jax.nn.sigmoid(gate_rows.astype(jnp.float32))
    return scaled.astype(jnp.bfloat16).reshape(SEQ_STEPS, HEADS_IN_SET * DV)

def project(head_a, head_b, emission_matrix_alpha, emission_matrix_beta):
    slice_rows = HEADS_IN_SET * DV // N_TP
    pieces_a = head_a.reshape(SEQ_STEPS, N_TP, slice_rows)
    pieces_b = head_b.reshape(SEQ_STEPS, N_TP, slice_rows)
    weights_a = emission_matrix_alpha.reshape(N_TP, slice_rows, D)
    weights_b = emission_matrix_beta.reshape(N_TP, slice_rows, D)

    def add_slice(slice_index, running_sum):
        slice_sum = jnp.dot(pieces_a[:, slice_index], weights_a[slice_index], preferred_element_type=jnp.float32)
        slice_sum = slice_sum + jnp.dot(pieces_b[:, slice_index], weights_b[slice_index], preferred_element_type=jnp.float32)
        return running_sum + lax.optimization_barrier(slice_sum.astype(jnp.bfloat16)).astype(jnp.float32)
    return lax.fori_loop(0, N_TP, add_slice, jnp.zeros((SEQ_STEPS, D), jnp.float32))

def expert_mixture(normed, dispatcher_columns, switch_matrix, expansion_matrix, contraction_matrix, item_specialist_cluster):
    sorted_order = jnp.argsort(item_specialist_cluster, stable=True).astype(jnp.int32)
    members = item_specialist_cluster[None, :] == jnp.arange(GROUPS, dtype=jnp.int32)[:, None]
    counts = lax.optimization_barrier(jnp.sum(members.astype(jnp.int32), axis=1))
    starts = jnp.cumsum(counts) - counts
    group_slots = SEQ_STEPS // ROWS_DEV * CAP
    slice_width = EXP_GROUP * FF // N_TP

    def one_group(group):
        slot_index = jnp.arange(group_slots, dtype=jnp.int32)
        filled = slot_index < counts[group]
        token_index = sorted_order[jnp.minimum(starts[group] + slot_index, SEQ_STEPS - 1)]
        group_rows = jnp.where(filled[:, None], normed[token_index], jnp.zeros((), jnp.bfloat16))
        columns = lax.dynamic_slice_in_dim(dispatcher_columns, group * EXP_GROUP, EXP_GROUP, 1)
        scores = jax.nn.sigmoid(jnp.dot(group_rows, columns, preferred_element_type=jnp.float32))
        weights = scores / lax.optimization_barrier(jnp.sum(scores, axis=1, keepdims=True))
        gate_proj = jnp.dot(group_rows, switch_matrix[group], preferred_element_type=jnp.float32)
        up_proj = jnp.dot(group_rows, expansion_matrix[group], preferred_element_type=jnp.float32)
        hidden = (jax.nn.silu(gate_proj) * up_proj).astype(jnp.bfloat16)
        down_rows = contraction_matrix[group]

        def add_slice(slice_index, running_sum):
            first_unit = (slice_index * slice_width).astype(jnp.int32)
            hidden_part = lax.dynamic_slice_in_dim(hidden, first_unit, slice_width, 1)
            down_part = lax.dynamic_slice_in_dim(down_rows, first_unit, slice_width, 0)
            product = jnp.dot(hidden_part, down_part, preferred_element_type=jnp.float32)
            member = (first_unit // FF).astype(jnp.int32)
            member_weight = lax.dynamic_slice_in_dim(weights, member, 1, 1)
            slice_sum = member_weight * product
            return running_sum + lax.optimization_barrier(slice_sum.astype(jnp.bfloat16)).astype(jnp.float32)
        running_sum = lax.fori_loop(0, N_TP, add_slice, jnp.zeros((group_slots, D), jnp.float32))
        return (running_sum.astype(jnp.bfloat16), jnp.where(filled, token_index, SEQ_STEPS))
    routed_rows, targets = lax.map(one_group, jnp.arange(GROUPS, dtype=jnp.int32))
    empty = jnp.zeros((SEQ_STEPS, D), jnp.bfloat16)
    return empty.at[targets.reshape(-1)].set(routed_rows.reshape(-1, D), mode='drop')

def reference(ask_preactivation_left, keep_preactivation_left, keep_bound_complement_left, ask_preactivation_right, keep_preactivation_right, keep_bound_complement_right, payload_entries, emission_switch_logits, added_log_keep_bias, lanewise_rescale, emission_matrix_alpha, emission_matrix_beta, skip_stream, postrecurrence_rescale, premixture_rescale, postmixture_rescale, dispatcher_columns, switch_matrix, expansion_matrix, contraction_matrix, item_specialist_cluster):
    routing_assignment = added_log_keep_bias.reshape(SEQ_STEPS, HEADS_IN_SET, 2)
    content_coupling = payload_entries.astype(jnp.float32).reshape(SEQ_STEPS, HEADS_IN_SET, 2, DV)
    gate_pair = emission_switch_logits.reshape(SEQ_STEPS, HEADS_IN_SET, 2, DV)
    raw_leading_factor = partitioned_result_array(ask_preactivation_left, keep_preactivation_left, keep_bound_complement_left, routing_assignment[:, :, 0], content_coupling[:, :, 0])
    raw_trailing_factor = partitioned_result_array(ask_preactivation_right, keep_preactivation_right, keep_bound_complement_right, routing_assignment[:, :, 1], content_coupling[:, :, 1])
    head_a = head_rows(raw_leading_factor, gate_pair[:, :, 0], lanewise_rescale)
    head_b = head_rows(raw_trailing_factor, gate_pair[:, :, 1], lanewise_rescale)
    mixed = project(head_a, head_b, emission_matrix_alpha, emission_matrix_beta)
    h_mid = (skip_stream.astype(jnp.float32) + rms_scale(mixed, postrecurrence_rescale)).astype(jnp.bfloat16)
    normed = rms_scale(h_mid.astype(jnp.float32), premixture_rescale).astype(jnp.bfloat16)
    routed = expert_mixture(normed, dispatcher_columns, switch_matrix, expansion_matrix, contraction_matrix, item_specialist_cluster)
    return (h_mid.astype(jnp.float32) + rms_scale(routed.astype(jnp.float32), postmixture_rescale)).astype(jnp.bfloat16)
```

```python
import functools

import jax
import jax.numpy as jnp
from jax import lax
from jax.experimental import pallas as pl
from jax.experimental.pallas import tpu as pltpu
from jax.sharding import PartitionSpec as P

FF = 2048
EPSILON = 1e-06


def rms_scale(features, gain):
    return (
        features * lax.rsqrt(jnp.mean(features * features, axis=-1, keepdims=True) + EPSILON) * gain
    )


MESH_ID = pl.DeviceIdType.MESH
NT = (((1,), (1,)), ((), ()))
TN = (((0,), (0,)), ((), ()))


def mixer_kernel(
    n_sp, heads, ka, kb, dv,
    qa, fa, ga, qb, fb, gb, val, gate, bias, gain,
    out,
    msg, inbox, carry, qda, qdb, kga, kgb, raw, send_sem, recv_sem,
):
    place = lax.axis_index("sp")
    barrier = pltpu.get_barrier_semaphore()
    for k in range(1, n_sp):
        pl.semaphore_signal(
            barrier, inc=1, device_id={"sp": lax.rem(place + k, n_sp)}, device_id_type=MESH_ID
        )
    rows = qa.shape[0]
    pair = 2 * dv
    width = ka + kb
    row_id = lax.broadcasted_iota(jnp.int32, (rows, rows), 0)
    col_id = lax.broadcasted_iota(jnp.int32, (rows, rows), 1)
    causal = row_id >= col_id
    tri = jnp.where(causal, 1.0, 0.0).astype(jnp.bfloat16)

    def prepare(q_ref, f_ref, g_ref, spike, k, h, qd_ref, kg_ref, at):
        lanes = pl.ds(h * k, k)
        q = q_ref[:, lanes].astype(jnp.float32)
        q = q / (1.0 + jnp.exp(-q))
        f = f_ref[:, lanes].astype(jnp.float32)
        key = g_ref[:, lanes] / (1.0 + jnp.exp(f))
        logf = jnp.log1p(-key) + spike
        high = logf.astype(jnp.bfloat16)
        low = (logf - high.astype(jnp.float32)).astype(jnp.bfloat16)
        inside = jnp.dot(tri, high, preferred_element_type=jnp.float32) + jnp.dot(
            tri, low, preferred_element_type=jnp.float32
        )
        total = inside[rows - 1 : rows, :]
        kg = (key * jnp.exp(-inside)).astype(jnp.bfloat16)
        qd_ref[:, lanes] = (q * jnp.exp(inside)).astype(jnp.bfloat16)
        kg_ref[:, lanes] = kg
        v = val[:, pl.ds((at // width) * pair, pair)]
        state = lax.dot_general(v, kg, TN, preferred_element_type=jnp.float32)
        return total, state * jnp.exp(total)

    for h in range(heads):
        for g, (q_ref, f_ref, g_ref, k, qd, kg) in enumerate(
            ((qa, fa, ga, ka, qda, kga), (qb, fb, gb, kb, qdb, kgb))
        ):
            at = h * width + g * ka
            spike = bias[:, 2 * h + g : 2 * h + g + 1]
            total, state = prepare(q_ref, f_ref, g_ref, spike, k, h, qd, kg, at)
            high = total.astype(jnp.bfloat16)
            low = (total - high.astype(jnp.float32)).astype(jnp.bfloat16)
            msg[:dv, at : at + k] = state[g * dv : (g + 1) * dv].astype(jnp.bfloat16)
            first = lax.broadcasted_iota(jnp.int32, (16, k), 0) == 0
            msg[dv:, at : at + k] = jnp.where(first, high, low)

    pl.semaphore_wait(barrier, n_sp - 1)

    def copy_to(k):
        return pltpu.make_async_remote_copy(
            src_ref=msg, dst_ref=inbox.at[place], send_sem=send_sem.at[k],
            recv_sem=recv_sem.at[place], device_id={"sp": lax.rem(place + k, n_sp)},
            device_id_type=MESH_ID,
        )

    for k in range(1, n_sp):
        @pl.when(place + k < n_sp)
        def _():
            copy_to(k).start()

    lane = lax.broadcasted_iota(jnp.int32, (rows, pair), 1)

    def scored(qd, kg, v):
        scores = lax.dot_general(qd, kg, NT, preferred_element_type=jnp.float32)
        scores = jnp.where(causal, scores, 0.0).astype(jnp.bfloat16)
        return jnp.dot(scores, v, preferred_element_type=jnp.float32)

    for h in range(heads):
        v = val[:, h * pair : (h + 1) * pair]
        out_a = scored(qda[:, h * ka : (h + 1) * ka], kga[:, h * ka : (h + 1) * ka], v)
        out_b = scored(qdb[:, h * kb : (h + 1) * kb], kgb[:, h * kb : (h + 1) * kb], v)
        raw[:, h * pair : (h + 1) * pair] = jnp.where(lane < dv, out_a, out_b)

    carry[...] = jnp.zeros_like(carry)
    for j in range(n_sp - 1):
        @pl.when(j < place)
        def _():
            pltpu.make_async_remote_copy(
                src_ref=msg, dst_ref=inbox.at[j], send_sem=send_sem.at[0],
                recv_sem=recv_sem.at[j], device_id={"sp": place}, device_id_type=MESH_ID,
            ).wait_recv()
            total = inbox[j, dv : dv + 1, :].astype(jnp.float32) + inbox[
                j, dv + 1 : dv + 2, :
            ].astype(jnp.float32)
            carry[...] = jnp.exp(total) * carry[...] + inbox[j, :dv, :].astype(jnp.float32)

    gains = jnp.concatenate([gain[...], gain[...]], axis=1)
    for h in range(heads):
        c = carry[:, h * width : (h + 1) * width].astype(jnp.bfloat16)
        zero_a = jnp.zeros((dv, ka), jnp.bfloat16)
        zero_b = jnp.zeros((dv, kb), jnp.bfloat16)
        state_a = jnp.concatenate([c[:, :ka], zero_a], axis=0)
        state_b = jnp.concatenate([zero_b, c[:, ka:]], axis=0)
        cols = slice(h * pair, (h + 1) * pair)
        x = raw[:, cols]
        x = x + lax.dot_general(
            qda[:, h * ka : (h + 1) * ka], state_a, NT, preferred_element_type=jnp.float32
        )
        x = x + lax.dot_general(
            qdb[:, h * kb : (h + 1) * kb], state_b, NT, preferred_element_type=jnp.float32
        )
        squares = x * x
        sum_a = jnp.sum(jnp.where(lane < dv, squares, 0.0), axis=1, keepdims=True)
        sum_b = jnp.sum(jnp.where(lane < dv, 0.0, squares), axis=1, keepdims=True)
        scale = lax.rsqrt(jnp.where(lane < dv, sum_a, sum_b) * (1.0 / dv) + EPSILON)
        open_gate = 1.0 / (1.0 + jnp.exp(-gate[:, cols].astype(jnp.float32)))
        out[:, cols] = (x * scale * gains * open_gate).astype(jnp.bfloat16)

    for k in range(1, n_sp):
        @pl.when(place + k < n_sp)
        def _():
            copy_to(k).wait_send()


def mixer(qa, fa, ga, qb, fb, gb, val, gate, bias, gain):
    n_sp = lax.axis_size("sp")
    rows = qa.shape[0]
    heads = bias.shape[1] // 2
    ka, kb = qa.shape[1] // heads, qb.shape[1] // heads
    dv = gain.shape[0]
    width = ka + kb
    bf, f32 = jnp.bfloat16, jnp.float32
    vm = pl.BlockSpec(memory_space=pltpu.VMEM)
    return pl.pallas_call(
        functools.partial(mixer_kernel, n_sp, heads, ka, kb, dv),
        out_shape=jax.ShapeDtypeStruct(val.shape, bf),
        in_specs=[vm] * 10,
        out_specs=vm,
        scratch_shapes=[
            pltpu.VMEM((dv + 16, heads * width), bf),
            pltpu.VMEM((n_sp, dv + 16, heads * width), bf),
            pltpu.VMEM((dv, heads * width), f32),
            pltpu.VMEM(qa.shape, bf),
            pltpu.VMEM(qb.shape, bf),
            pltpu.VMEM(qa.shape, bf),
            pltpu.VMEM(qb.shape, bf),
            pltpu.VMEM(val.shape, f32),
            pltpu.SemaphoreType.DMA((n_sp,)),
            pltpu.SemaphoreType.DMA((n_sp,)),
        ],
        compiler_params=pltpu.CompilerParams(
            collective_id=0, has_side_effects=True, vmem_limit_bytes=48 << 20
        ),
        name="mixer",
    )(qa, fa, ga.reshape(1, -1), qb, fb, gb.reshape(1, -1), val, gate, bias, gain.reshape(1, -1))


def expert_rows(
    piece, dispatcher_columns, switch_matrix, expansion_matrix, contraction_matrix, member
):
    flat_rows = piece.reshape(-1, piece.shape[-1])
    scores = jax.nn.sigmoid(
        jnp.dot(flat_rows, dispatcher_columns, preferred_element_type=jnp.float32)
    )
    weights = scores / jnp.sum(scores, axis=1, keepdims=True)
    picked = (
        lax.broadcasted_iota(jnp.int32, (1, dispatcher_columns.shape[1]), 1) == member
    ).astype(jnp.float32)
    member_weight = jnp.sum(weights * picked, axis=1, keepdims=True)
    gate_proj = jnp.dot(flat_rows, switch_matrix[0], preferred_element_type=jnp.float32)
    up_proj = jnp.dot(flat_rows, expansion_matrix[0], preferred_element_type=jnp.float32)
    hidden = (jax.nn.silu(gate_proj) * up_proj).astype(jnp.bfloat16)
    product = jnp.dot(hidden, contraction_matrix[0], preferred_element_type=jnp.float32)
    return (member_weight * product).astype(jnp.bfloat16).reshape(piece.shape)


def shards(
    ask_preactivation_left,
    keep_preactivation_left,
    keep_bound_complement_left,
    ask_preactivation_right,
    keep_preactivation_right,
    keep_bound_complement_right,
    payload_entries,
    emission_switch_logits,
    added_log_keep_bias,
    lanewise_rescale,
    emission_matrix_alpha,
    emission_matrix_beta,
    skip_stream,
    postrecurrence_rescale,
    premixture_rescale,
    postmixture_rescale,
    dispatcher_columns,
    switch_matrix,
    expansion_matrix,
    contraction_matrix,
    item_specialist_cluster,
):
    heads = mixer(
        ask_preactivation_left,
        keep_preactivation_left,
        keep_bound_complement_left,
        ask_preactivation_right,
        keep_preactivation_right,
        keep_bound_complement_right,
        payload_entries,
        emission_switch_logits,
        added_log_keep_bias,
        lanewise_rescale,
    )
    row_count = skip_stream.shape[0]
    value_width = lanewise_rescale.shape[0]
    weights = jnp.stack(
        [
            emission_matrix_alpha.reshape(-1, value_width, skip_stream.shape[1]),
            emission_matrix_beta.reshape(-1, value_width, skip_stream.shape[1]),
        ],
        axis=1,
    ).reshape(-1, skip_stream.shape[1])
    term = jnp.dot(heads, weights, preferred_element_type=jnp.float32)
    mixed = lax.psum_scatter(
        lax.optimization_barrier(term.astype(jnp.bfloat16))
        .astype(jnp.float32)
        .astype(jnp.bfloat16),
        "tp",
        scatter_dimension=0,
        tiled=True,
    ).astype(jnp.float32)
    h_mid = (skip_stream.astype(jnp.float32) + rms_scale(mixed, postrecurrence_rescale)).astype(
        jnp.bfloat16
    )
    normed = rms_scale(h_mid.astype(jnp.float32), premixture_rescale).astype(jnp.bfloat16)
    groups = lax.axis_size("sp")
    capacity = (9 * row_count + 8 * groups - 1) // (8 * groups)
    member = item_specialist_cluster[:, None] == lax.broadcasted_iota(
        jnp.int32, (row_count, groups), 1
    )
    member_count = member.astype(jnp.int32)
    slot_rank = jnp.sum(jnp.cumsum(member_count, axis=0) * member_count, axis=1) - 1
    slot_id = item_specialist_cluster * capacity + slot_rank
    placing = (
        slot_id[None, :] == lax.broadcasted_iota(jnp.int32, (groups * capacity, row_count), 0)
    ).astype(jnp.bfloat16)
    outgoing = jnp.dot(placing, normed, preferred_element_type=jnp.float32).astype(jnp.bfloat16)
    outgoing = outgoing.reshape(groups, capacity, normed.shape[1])
    incoming = lax.all_to_all(outgoing, "sp", split_axis=0, concat_axis=0, tiled=True)
    own_member = lax.axis_index("tp") * switch_matrix.shape[2] // FF
    partials = expert_rows(
        lax.all_gather(incoming, "tp", axis=0, tiled=True),
        dispatcher_columns,
        switch_matrix,
        expansion_matrix,
        contraction_matrix,
        own_member,
    )
    summed = lax.psum_scatter(
        partials.astype(jnp.float32).astype(jnp.bfloat16), "tp", scatter_dimension=0, tiled=True
    )
    returned = lax.all_to_all(summed, "sp", split_axis=0, concat_axis=0, tiled=True)
    routed = jnp.einsum(
        "sr,sd->rd",
        placing,
        returned.reshape(groups * capacity, -1),
        preferred_element_type=jnp.float32,
    )
    return (h_mid.astype(jnp.float32) + rms_scale(routed, postmixture_rescale)).astype(jnp.bfloat16)


def solution(mesh):
    placed = (
        P("sp", "tp"),
        P("sp", "tp"),
        P("tp"),
        P("sp", "tp"),
        P("sp", "tp"),
        P("tp"),
        P("sp", "tp"),
        P("sp", "tp"),
        P("sp", "tp"),
        P(),
        P("tp", None),
        P("tp", None),
        P(("sp", "tp"), None),
        P(),
        P(),
        P(),
        P(None, "sp"),
        P("sp", None, "tp"),
        P("sp", None, "tp"),
        P("sp", "tp", None),
        P(("sp", "tp")),
    )
    return jax.shard_map(
        shards, mesh=mesh, in_specs=placed, out_specs=P(("sp", "tp"), None), check_vma=False
    )
```

```python
import functools

import jax
import jax.numpy as jnp
from jax import lax
from jax.experimental import pallas as pl
from jax.experimental.pallas import tpu as pltpu
from jax.sharding import PartitionSpec as P

FF = 2048
EPSILON = 1e-06


def rms_scale(features, gain):
    return (
        features * lax.rsqrt(jnp.mean(features * features, axis=-1, keepdims=True) + EPSILON) * gain
    )


MESH_ID = pl.DeviceIdType.MESH
NT = (((1,), (1,)), ((), ()))
TN = (((0,), (0,)), ((), ()))


def mixer_kernel(
    n_sp, heads, ka, kb, dv,
    qa, fa, ga, qb, fb, gb, val, gate, bias, gain,
    out,
    msg, inbox, carry, qda, qdb, kga, kgb, raw, send_sem, recv_sem,
):
    place = lax.axis_index("sp")
    barrier = pltpu.get_barrier_semaphore()
    for k in range(1, n_sp):
        pl.semaphore_signal(
            barrier, inc=1, device_id={"sp": lax.rem(place + k, n_sp)}, device_id_type=MESH_ID
        )
    rows = qa.shape[0]
    pair = 2 * dv
    width = ka + kb
    row_id = lax.broadcasted_iota(jnp.int32, (rows, rows), 0)
    col_id = lax.broadcasted_iota(jnp.int32, (rows, rows), 1)
    causal = row_id >= col_id
    tri = jnp.where(causal, 1.0, 0.0).astype(jnp.bfloat16)

    def prepare(q_ref, f_ref, g_ref, spike, k, h, qd_ref, kg_ref, at):
        lanes = pl.ds(h * k, k)
        q = q_ref[:, lanes].astype(jnp.float32)
        q = q / (1.0 + jnp.exp(-q))
        f = f_ref[:, lanes].astype(jnp.float32)
        key = g_ref[:, lanes] / (1.0 + jnp.exp(f))
        logf = jnp.log1p(-key) + spike
        high = logf.astype(jnp.bfloat16)
        low = (logf - high.astype(jnp.float32)).astype(jnp.bfloat16)
        inside = jnp.dot(tri, high, preferred_element_type=jnp.float32) + jnp.dot(
            tri, low, preferred_element_type=jnp.float32
        )
        total = inside[rows - 1 : rows, :]
        kg = (key * jnp.exp(-inside)).astype(jnp.bfloat16)
        qd_ref[:, lanes] = (q * jnp.exp(inside)).astype(jnp.bfloat16)
        kg_ref[:, lanes] = kg
        v = val[:, pl.ds((at // width) * pair, pair)]
        state = lax.dot_general(v, kg, TN, preferred_element_type=jnp.float32)
        return total, state * jnp.exp(total)

    for h in range(heads):
        for g, (q_ref, f_ref, g_ref, k, qd, kg) in enumerate(
            ((qa, fa, ga, ka, qda, kga), (qb, fb, gb, kb, qdb, kgb))
        ):
            at = h * width + g * ka
            spike = bias[:, 2 * h + g : 2 * h + g + 1]
            total, state = prepare(q_ref, f_ref, g_ref, spike, k, h, qd, kg, at)
            high = total.astype(jnp.bfloat16)
            low = (total - high.astype(jnp.float32)).astype(jnp.bfloat16)
            msg[:dv, at : at + k] = state[g * dv : (g + 1) * dv].astype(jnp.bfloat16)
            first = lax.broadcasted_iota(jnp.int32, (16, k), 0) == 0
            msg[dv:, at : at + k] = jnp.where(first, high, low)

    pl.semaphore_wait(barrier, n_sp - 1)

    def copy_to(k):
        return pltpu.make_async_remote_copy(
            src_ref=msg, dst_ref=inbox.at[place], send_sem=send_sem.at[k],
            recv_sem=recv_sem.at[place], device_id={"sp": lax.rem(place + k, n_sp)},
            device_id_type=MESH_ID,
        )

    for k in range(1, n_sp):
        @pl.when(place + k < n_sp)
        def _():
            copy_to(k).start()

    lane = lax.broadcasted_iota(jnp.int32, (rows, pair), 1)

    def scored(qd, kg, v):
        scores = lax.dot_general(qd, kg, NT, preferred_element_type=jnp.float32)
        scores = jnp.where(causal, scores, 0.0).astype(jnp.bfloat16)
        return jnp.dot(scores, v, preferred_element_type=jnp.float32)

    for h in range(heads):
        v = val[:, h * pair : (h + 1) * pair]
        out_a = scored(qda[:, h * ka : (h + 1) * ka], kga[:, h * ka : (h + 1) * ka], v)
        out_b = scored(qdb[:, h * kb : (h + 1) * kb], kgb[:, h * kb : (h + 1) * kb], v)
        raw[:, h * pair : (h + 1) * pair] = jnp.where(lane < dv, out_a, out_b)

    carry[...] = jnp.zeros_like(carry)
    for j in range(n_sp - 1):
        @pl.when(j < place)
        def _():
            pltpu.make_async_remote_copy(
                src_ref=msg, dst_ref=inbox.at[j], send_sem=send_sem.at[0],
                recv_sem=recv_sem.at[j], device_id={"sp": place}, device_id_type=MESH_ID,
            ).wait_recv()
            total = inbox[j, dv : dv + 1, :].astype(jnp.float32) + inbox[
                j, dv + 1 : dv + 2, :
            ].astype(jnp.float32)
            carry[...] = jnp.exp(total) * carry[...] + inbox[j, :dv, :].astype(jnp.float32)

    gains = jnp.concatenate([gain[...], gain[...]], axis=1)
    for h in range(heads):
        c = carry[:, h * width : (h + 1) * width].astype(jnp.bfloat16)
        zero_a = jnp.zeros((dv, ka), jnp.bfloat16)
        zero_b = jnp.zeros((dv, kb), jnp.bfloat16)
        state_a = jnp.concatenate([c[:, :ka], zero_a], axis=0)
        state_b = jnp.concatenate([zero_b, c[:, ka:]], axis=0)
        cols = slice(h * pair, (h + 1) * pair)
        x = raw[:, cols]
        x = x + lax.dot_general(
            qda[:, h * ka : (h + 1) * ka], state_a, NT, preferred_element_type=jnp.float32
        )
        x = x + lax.dot_general(
            qdb[:, h * kb : (h + 1) * kb], state_b, NT, preferred_element_type=jnp.float32
        )
        squares = x * x
        sum_a = jnp.sum(jnp.where(lane < dv, squares, 0.0), axis=1, keepdims=True)
        sum_b = jnp.sum(jnp.where(lane < dv, 0.0, squares), axis=1, keepdims=True)
        scale = lax.rsqrt(jnp.where(lane < dv, sum_a, sum_b) * (1.0 / dv) + EPSILON)
        open_gate = 1.0 / (1.0 + jnp.exp(-gate[:, cols].astype(jnp.float32)))
        out[:, cols] = (x * scale * gains * open_gate).astype(jnp.bfloat16)

    for k in range(1, n_sp):
        @pl.when(place + k < n_sp)
        def _():
            copy_to(k).wait_send()


def mixer(qa, fa, ga, qb, fb, gb, val, gate, bias, gain):
    n_sp = lax.axis_size("sp")
    rows = qa.shape[0]
    heads = bias.shape[1] // 2
    ka, kb = qa.shape[1] // heads, qb.shape[1] // heads
    dv = gain.shape[0]
    width = ka + kb
    bf, f32 = jnp.bfloat16, jnp.float32
    vm = pl.BlockSpec(memory_space=pltpu.VMEM)
    return pl.pallas_call(
        functools.partial(mixer_kernel, n_sp, heads, ka, kb, dv),
        out_shape=jax.ShapeDtypeStruct(val.shape, bf),
        in_specs=[vm] * 10,
        out_specs=vm,
        scratch_shapes=[
            pltpu.VMEM((dv + 16, heads * width), bf),
            pltpu.VMEM((n_sp, dv + 16, heads * width), bf),
            pltpu.VMEM((dv, heads * width), f32),
            pltpu.VMEM(qa.shape, bf),
            pltpu.VMEM(qb.shape, bf),
            pltpu.VMEM(qa.shape, bf),
            pltpu.VMEM(qb.shape, bf),
            pltpu.VMEM(val.shape, f32),
            pltpu.SemaphoreType.DMA((n_sp,)),
            pltpu.SemaphoreType.DMA((n_sp,)),
        ],
        compiler_params=pltpu.CompilerParams(
            collective_id=0, has_side_effects=True, vmem_limit_bytes=48 << 20
        ),
        name="mixer",
    )(qa, fa, ga.reshape(1, -1), qb, fb, gb.reshape(1, -1), val, gate, bias, gain.reshape(1, -1))


def landed(ref, sem, source):
    pltpu.make_async_remote_copy(
        src_ref=ref, dst_ref=ref, send_sem=sem, recv_sem=sem, device_id=source,
        device_id_type=MESH_ID,
    ).wait_recv()


def line_reduce(z, core, nz, rows, part, twin, box_r, box_l, out_r, out_l, sems, to_right, to_left):
    twin_recv, send_r, recv_r, send_l, recv_l = sems
    chunks = part.shape[1]
    own = pl.ds(pl.multiple_of(core * rows, rows), rows)

    def base(d, ch):
        return part[d, ch, own, :].astype(jnp.float32) + twin[d, ch].astype(jnp.float32)

    def twin_wait(d):
        landed(twin.at[d], twin_recv.at[d], to_right)

    def hop(out, box, send, recv, d, ch, to):
        return pltpu.make_async_remote_copy(
            src_ref=out.at[d, ch], dst_ref=box.at[d, ch], send_sem=send.at[d, ch],
            recv_sem=recv.at[d, ch], device_id=to, device_id_type=MESH_ID,
        )

    def side(d, has_in, out, box, send, recv, to):
        twin_wait(d)
        for ch in range(chunks):
            @pl.when(has_in)
            def _():
                hop(out, box, send, recv, d, ch, to).wait_recv()
                total = base(d, ch) + box[d, ch].astype(jnp.float32)
                out[d, ch] = total.astype(jnp.bfloat16)

            @pl.when(jnp.logical_not(has_in))
            def _():
                out[d, ch] = base(d, ch).astype(jnp.bfloat16)

            hop(out, box, send, recv, d, ch, to).start()

    def step(tau, _):
        @pl.when((tau >= z) & (z < nz - 1))
        def _():
            side(nz - 1 + z - tau, z > 0, out_r, box_r, send_r, recv_r, to_right)

        @pl.when((tau + z >= nz - 1) & (z > 0))
        def _():
            side(tau + z - (nz - 1), z < nz - 1, out_l, box_l, send_l, recv_l, to_left)

        return 0

    lax.fori_loop(0, nz - 1, step, 0)

    def finish(total):
        twin_wait(z)
        for ch in range(chunks):
            total[ch] = base(z, ch)

            @pl.when(z > 0)
            def _():
                hop(out_r, box_r, send_r, recv_r, z, ch, to_right).wait_recv()
                total[ch] = total[ch] + box_r[z, ch].astype(jnp.float32)

            @pl.when(z < nz - 1)
            def _():
                hop(out_l, box_l, send_l, recv_l, z, ch, to_left).wait_recv()
                total[ch] = total[ch] + box_l[z, ch].astype(jnp.float32)

    def drain():
        def one(d, _):
            for ch in range(chunks):
                @pl.when(d > z)
                def _():
                    hop(out_r, box_r, send_r, recv_r, d, ch, to_right).wait_send()

                @pl.when(d < z)
                def _():
                    hop(out_l, box_l, send_l, recv_l, d, ch, to_left).wait_send()

            return 0

        lax.fori_loop(0, nz, one, 0)

    return finish, drain


def experts_kernel(
    dv, n_sp, nz, cap, pad,
    heads, alpha, beta, skip, gain1, gain2, gain3, router, w1, w2, w3, cluster,
    out,
    wcat, w1v, w2v, w3v, part, twin, box_r, box_l, out_r, out_l, mixed, hmid, placing,
    sp_out, sp_in, xs, part2, twin2, box_r2, box_l2, out_r2, out_l2, summed, back_out, back_in,
    wsem, tw_s, tw_r, rs_sr, rs_rr, rs_sl, rs_rl, sp_s, sp_r,
    ag_sr, ag_rr, ag_sl, ag_rl, ag_ds, ag_dr,
    tw2_s, tw2_r, rs2_sr, rs2_rr, rs2_sl, rs2_rl, bk_s, bk_r,
):
    f32, bf = jnp.float32, jnp.bfloat16
    place, t = lax.axis_index("sp"), lax.axis_index("tp")
    z, core = t // 2, t % 2
    peer = {"tp": z * 2 + 1 - core}
    to_right = {"tp": jnp.minimum(z + 1, nz - 1) * 2 + core}
    to_left = {"tp": jnp.maximum(z - 1, 0) * 2 + core}

    barrier = pltpu.get_barrier_semaphore()
    for k in range(1, n_sp):
        pl.semaphore_signal(
            barrier, inc=1, device_id={"sp": lax.rem(place + k, n_sp)}, device_id_type=MESH_ID
        )
    pl.semaphore_signal(barrier, inc=1, device_id=peer, device_id_type=MESH_ID)

    @pl.when(z < nz - 1)
    def _():
        pl.semaphore_signal(barrier, inc=1, device_id=to_right, device_id_type=MESH_ID)

    @pl.when(z > 0)
    def _():
        pl.semaphore_signal(barrier, inc=1, device_id=to_left, device_id_type=MESH_ID)

    loads = [
        pltpu.make_async_copy(src.at[0], dst, wsem.at[i])
        for i, (src, dst) in enumerate(((w1, w1v), (w2, w2v), (w3, w3v)))
    ]
    for load in loads:
        load.start()

    rows, width = skip.shape
    chunks = part.shape[1]
    half = width // chunks
    slots = n_sp * pad
    compact = xs.shape[2] // 2
    for h in range(alpha.shape[0] // dv):
        wcat[2 * h * dv : (2 * h + 1) * dv] = alpha[h * dv : (h + 1) * dv]
        wcat[(2 * h + 1) * dv : (2 * h + 2) * dv] = beta[h * dv : (h + 1) * dv]

    pl.semaphore_wait(
        barrier,
        n_sp + jnp.where(z > 0, 1, 0) + jnp.where(z < nz - 1, 1, 0),
    )

    def twin_copy(src, dst, d, size, send, recv):
        theirs = pl.ds(pl.multiple_of((1 - core) * size, size), size)
        return pltpu.make_async_remote_copy(
            src_ref=src.at[d, :, theirs, :], dst_ref=dst.at[d], send_sem=send.at[d],
            recv_sem=recv.at[d], device_id=peer, device_id_type=MESH_ID,
        )

    def project(i, _):
        d = jnp.where(i % 2 == 0, nz - 1 - i // 2, i // 2)
        x = heads[pl.ds(pl.multiple_of(d * 2 * rows, 2 * rows), 2 * rows), :]
        for ch in range(chunks):
            part[d, ch] = jnp.dot(
                x, wcat[:, ch * half : (ch + 1) * half], preferred_element_type=f32
            ).astype(bf)
        twin_copy(part, twin, d, rows, tw_s, tw_r).start()
        return 0

    lax.fori_loop(0, nz, project, 0)
    finish, drain = line_reduce(
        z, core, nz, rows, part, twin, box_r, box_l, out_r, out_l,
        (tw_r, rs_sr, rs_rr, rs_sl, rs_rl), to_right, to_left,
    )
    finish(mixed)

    def whole(ref):
        return jnp.concatenate([ref[ch] for ch in range(chunks)], axis=1)

    mid = skip[...].astype(f32) + rms_scale(whole(mixed), gain1[...])
    hmid[...] = mid.astype(bf)
    normed = rms_scale(hmid[...].astype(f32), gain2[...]).astype(bf)

    group = cluster[...]
    onehot = lax.broadcasted_iota(jnp.int32, (n_sp, rows), 0) == group
    ones = jnp.where(onehot, 1.0, 0.0)
    upto = jnp.where(
        lax.broadcasted_iota(jnp.int32, (rows, rows), 0)
        <= lax.broadcasted_iota(jnp.int32, (rows, rows), 1),
        1.0,
        0.0,
    ).astype(bf)
    counts = jnp.dot(ones.astype(bf), upto, preferred_element_type=f32)
    rank = jnp.sum(ones * counts, axis=0, keepdims=True).astype(jnp.int32) - 1
    slot = group * pad + rank
    placing[...] = jnp.where(
        lax.broadcasted_iota(jnp.int32, (slots, rows), 0) == slot, 1.0, 0.0
    ).astype(bf)
    col = lax.broadcasted_iota(jnp.int32, (compact, slots), 1)
    inner = col & (pad - 1)
    target = (col >> (pad.bit_length() - 1)) * cap + inner
    packing = jnp.where(
        (lax.broadcasted_iota(jnp.int32, (compact, slots), 0) == target) & (inner < cap), 1.0, 0.0
    ).astype(bf)

    def sp_copy(src, dst, k, send, recv):
        g = lax.rem(place + k, n_sp)
        return pltpu.make_async_remote_copy(
            src_ref=src.at[g], dst_ref=dst.at[place], send_sem=send.at[g],
            recv_sem=recv.at[place], device_id={"sp": g}, device_id_type=MESH_ID,
        )

    def sp_exchange(src, dst, send, recv):
        for k in range(1, n_sp):
            sp_copy(src, dst, k, send, recv).start()
        dst[place] = src[place]
        for k in range(1, n_sp):
            g = lax.rem(place + k, n_sp)
            landed(dst.at[g], recv.at[g], peer)

    sp_out[...] = (
        jnp.dot(placing[...], normed, preferred_element_type=f32)
        .astype(bf)
        .reshape(n_sp, pad, width)
    )
    sp_exchange(sp_out, sp_in, sp_s, sp_r)
    packed = jnp.dot(
        packing, sp_in[...].reshape(slots, width), preferred_element_type=f32
    ).astype(bf)
    mine = pl.ds(pl.multiple_of(core * compact, compact), compact)
    theirs = pl.ds(pl.multiple_of((1 - core) * compact, compact), compact)
    for ch in range(chunks):
        xs[z, ch, mine, :] = packed[:, ch * half : (ch + 1) * half]

    for load in loads:
        load.wait()

    def spread(d, ch, send, recv, to):
        return pltpu.make_async_remote_copy(
            src_ref=xs.at[d, ch, mine, :], dst_ref=xs.at[d, ch, mine, :],
            send_sem=send.at[d, ch], recv_sem=recv.at[d, ch], device_id=to,
            device_id_type=MESH_ID,
        )

    member = t * w1v.shape[1] // FF

    def expert(d):
        for ch in range(chunks):
            landed(xs.at[d, ch, theirs, :], ag_dr.at[d, ch], peer)
        gate = up = score = 0.0
        for ch in range(chunks):
            x = xs[d, ch]
            depth = pl.ds(ch * half, half)
            gate = gate + jnp.dot(x, w1v[depth, :], preferred_element_type=f32)
            up = up + jnp.dot(x, w2v[depth, :], preferred_element_type=f32)
            score = score + jnp.dot(x, router[depth, :], preferred_element_type=f32)
        score = 1.0 / (1.0 + jnp.exp(-score))
        picked = lax.broadcasted_iota(jnp.int32, score.shape, 1) == member
        weight = jnp.sum(jnp.where(picked, score, 0.0), axis=1, keepdims=True) / jnp.sum(
            score, axis=1, keepdims=True
        )
        hidden = (gate / (1.0 + jnp.exp(-gate)) * up).astype(bf)
        for ch in range(chunks):
            y = jnp.dot(hidden, w3v[:, ch * half : (ch + 1) * half], preferred_element_type=f32)
            part2[d, ch] = (weight * y).astype(bf)
        twin_copy(part2, twin2, d, compact, tw2_s, tw2_r).start()

    def gather(tau, _):
        low, high = z - tau, z + tau
        for ch in range(chunks):
            @pl.when(low >= 0)
            def _():
                @pl.when(tau > 0)
                def _():
                    spread(low, ch, ag_sr, ag_rr, to_right).wait_recv()

                @pl.when(z < nz - 1)
                def _():
                    spread(low, ch, ag_sr, ag_rr, to_right).start()

                spread(low, ch, ag_ds, ag_dr, peer).start()

            @pl.when(high < nz)
            def _():
                @pl.when(tau > 0)
                def _():
                    spread(high, ch, ag_sl, ag_rl, to_left).wait_recv()

                @pl.when(z > 0)
                def _():
                    spread(high, ch, ag_sl, ag_rl, to_left).start()

                @pl.when(tau > 0)
                def _():
                    spread(high, ch, ag_ds, ag_dr, peer).start()

        @pl.when(low >= 0)
        def _():
            expert(low)

        @pl.when((high < nz) & (tau > 0))
        def _():
            expert(high)

        return 0

    lax.fori_loop(0, nz, gather, 0)
    finish2, drain2 = line_reduce(
        z, core, nz, compact, part2, twin2, box_r2, box_l2, out_r2, out_l2,
        (tw2_r, rs2_sr, rs2_rr, rs2_sl, rs2_rl), to_right, to_left,
    )
    finish2(summed)
    back_out[...] = (
        lax.dot_general(packing, whole(summed).astype(bf), TN, preferred_element_type=f32)
        .astype(bf)
        .reshape(n_sp, pad, width)
    )
    sp_exchange(back_out, back_in, bk_s, bk_r)
    routed = lax.dot_general(
        placing[...], back_in[...].reshape(slots, width), TN, preferred_element_type=f32
    )
    out[...] = (hmid[...].astype(f32) + rms_scale(routed, gain3[...])).astype(bf)

    drain()
    drain2()

    def settle(d, _):
        twin_copy(part, twin, d, rows, tw_s, tw_r).wait_send()
        twin_copy(part2, twin2, d, compact, tw2_s, tw2_r).wait_send()
        for ch in range(chunks):
            spread(d, ch, ag_ds, ag_dr, peer).wait_send()

            @pl.when((d <= z) & (z < nz - 1))
            def _():
                spread(d, ch, ag_sr, ag_rr, to_right).wait_send()

            @pl.when((d >= z) & (z > 0))
            def _():
                spread(d, ch, ag_sl, ag_rl, to_left).wait_send()

        return 0

    lax.fori_loop(0, nz, settle, 0)
    for k in range(1, n_sp):
        sp_copy(sp_out, sp_in, k, sp_s, sp_r).wait_send()
        sp_copy(back_out, back_in, k, bk_s, bk_r).wait_send()


def mixture(dv, heads, alpha, beta, skip, g1, g2, g3, router, w1, w2, w3, cluster):
    n_sp, nz = lax.axis_size("sp"), lax.axis_size("tp") // 2
    rows, width = skip.shape
    cap = (9 * rows + 8 * n_sp - 1) // (8 * n_sp)
    pad = 16
    while pad < cap:
        pad *= 2
    compact = (n_sp * cap + 15) // 16 * 16
    chunks, half = 2, width // 2
    f32, bf = jnp.float32, jnp.bfloat16
    vm = pl.BlockSpec(memory_space=pltpu.VMEM)
    hbm = pl.BlockSpec(memory_space=pl.ANY)
    line = (nz, chunks, rows, half)
    line2 = (nz, chunks, compact, half)
    dma = pltpu.SemaphoreType.DMA
    reduce_sems = [dma((nz,))] * 2 + [dma((nz, chunks))] * 4
    return pl.pallas_call(
        functools.partial(experts_kernel, dv, n_sp, nz, cap, pad),
        out_shape=jax.ShapeDtypeStruct(skip.shape, bf),
        in_specs=[vm] * 8 + [hbm] * 3 + [vm],
        out_specs=vm,
        scratch_shapes=[
            pltpu.VMEM((2 * alpha.shape[0], width), bf),
            pltpu.VMEM(w1.shape[1:], bf),
            pltpu.VMEM(w2.shape[1:], bf),
            pltpu.VMEM(w3.shape[1:], bf),
            pltpu.VMEM((nz, chunks, 2 * rows, half), bf),
        ]
        + [pltpu.VMEM(line, bf)] * 5
        + [
            pltpu.VMEM(line[1:], f32),
            pltpu.VMEM(skip.shape, bf),
            pltpu.VMEM((n_sp * pad, rows), bf),
            pltpu.VMEM((n_sp, pad, width), bf),
            pltpu.VMEM((n_sp, pad, width), bf),
            pltpu.VMEM((nz, chunks, 2 * compact, half), bf),
            pltpu.VMEM((nz, chunks, 2 * compact, half), bf),
        ]
        + [pltpu.VMEM(line2, bf)] * 5
        + [
            pltpu.VMEM(line2[1:], f32),
            pltpu.VMEM((n_sp, pad, width), bf),
            pltpu.VMEM((n_sp, pad, width), bf),
            dma((3,)),
        ]
        + reduce_sems
        + [dma((n_sp,))] * 2
        + [dma((nz, chunks))] * 6
        + reduce_sems
        + [dma((n_sp,))] * 2,
        compiler_params=pltpu.CompilerParams(
            collective_id=1, has_side_effects=True, vmem_limit_bytes=60 << 20
        ),
        name="mixture",
    )(
        heads, alpha, beta, skip, g1.reshape(1, -1), g2.reshape(1, -1), g3.reshape(1, -1),
        router, w1, w2, w3, cluster.reshape(1, -1),
    )


def shards(
    ask_preactivation_left,
    keep_preactivation_left,
    keep_bound_complement_left,
    ask_preactivation_right,
    keep_preactivation_right,
    keep_bound_complement_right,
    payload_entries,
    emission_switch_logits,
    added_log_keep_bias,
    lanewise_rescale,
    emission_matrix_alpha,
    emission_matrix_beta,
    skip_stream,
    postrecurrence_rescale,
    premixture_rescale,
    postmixture_rescale,
    dispatcher_columns,
    switch_matrix,
    expansion_matrix,
    contraction_matrix,
    item_specialist_cluster,
):
    heads = mixer(
        ask_preactivation_left,
        keep_preactivation_left,
        keep_bound_complement_left,
        ask_preactivation_right,
        keep_preactivation_right,
        keep_bound_complement_right,
        payload_entries,
        emission_switch_logits,
        added_log_keep_bias,
        lanewise_rescale,
    )
    return mixture(
        lanewise_rescale.shape[0],
        heads,
        emission_matrix_alpha,
        emission_matrix_beta,
        skip_stream,
        postrecurrence_rescale,
        premixture_rescale,
        postmixture_rescale,
        dispatcher_columns,
        switch_matrix,
        expansion_matrix,
        contraction_matrix,
        item_specialist_cluster,
    )


def solution(mesh):
    placed = (
        P("sp", "tp"),
        P("sp", "tp"),
        P("tp"),
        P("sp", "tp"),
        P("sp", "tp"),
        P("tp"),
        P("sp", "tp"),
        P("sp", "tp"),
        P("sp", "tp"),
        P(),
        P("tp", None),
        P("tp", None),
        P(("sp", "tp"), None),
        P(),
        P(),
        P(),
        P(None, "sp"),
        P("sp", None, "tp"),
        P("sp", None, "tp"),
        P("sp", "tp", None),
        P(("sp", "tp")),
    )
    return jax.shard_map(
        shards, mesh=mesh, in_specs=placed, out_specs=P(("sp", "tp"), None), check_vma=False
    )
```

```python
import functools

import jax
import jax.numpy as jnp
from jax import lax
from jax.experimental import pallas as pl
from jax.experimental.pallas import tpu as pltpu
from jax.sharding import PartitionSpec as P

FF = 2048
CHUNKS = 4
EPSILON = 1e-06


def rms_scale(features, gain):
    return (
        features * lax.rsqrt(jnp.mean(features * features, axis=-1, keepdims=True) + EPSILON) * gain
    )


MESH_ID = pl.DeviceIdType.MESH
NT = (((1,), (1,)), ((), ()))
TN = (((0,), (0,)), ((), ()))


def mixer_kernel(
    n_sp, heads, ka, kb, dv,
    qa, fa, ga, qb, fb, gb, val, gate, bias, gain,
    out,
    msg, inbox, carry, qda, qdb, kga, kgb, raw, send_sem, recv_sem,
):
    place = lax.axis_index("sp")
    barrier = pltpu.get_barrier_semaphore()
    for k in range(1, n_sp):
        pl.semaphore_signal(
            barrier, inc=1, device_id={"sp": lax.rem(place + k, n_sp)}, device_id_type=MESH_ID
        )
    rows = qa.shape[0]
    pair = 2 * dv
    width = ka + kb
    row_id = lax.broadcasted_iota(jnp.int32, (rows, rows), 0)
    col_id = lax.broadcasted_iota(jnp.int32, (rows, rows), 1)
    causal = row_id >= col_id
    tri = jnp.where(causal, 1.0, 0.0).astype(jnp.bfloat16)

    def prepare(q_ref, f_ref, g_ref, spike, k, h, qd_ref, kg_ref, at):
        lanes = pl.ds(h * k, k)
        q = q_ref[:, lanes].astype(jnp.float32)
        q = q / (1.0 + jnp.exp(-q))
        f = f_ref[:, lanes].astype(jnp.float32)
        key = g_ref[:, lanes] / (1.0 + jnp.exp(f))
        logf = jnp.log1p(-key) + spike
        high = logf.astype(jnp.bfloat16)
        low = (logf - high.astype(jnp.float32)).astype(jnp.bfloat16)
        inside = jnp.dot(tri, high, preferred_element_type=jnp.float32) + jnp.dot(
            tri, low, preferred_element_type=jnp.float32
        )
        total = inside[rows - 1 : rows, :]
        kg = (key * jnp.exp(-inside)).astype(jnp.bfloat16)
        qd_ref[:, lanes] = (q * jnp.exp(inside)).astype(jnp.bfloat16)
        kg_ref[:, lanes] = kg
        v = val[:, pl.ds((at // width) * pair, pair)]
        state = lax.dot_general(v, kg, TN, preferred_element_type=jnp.float32)
        return total, state * jnp.exp(total)

    for h in range(heads):
        for g, (q_ref, f_ref, g_ref, k, qd, kg) in enumerate(
            ((qa, fa, ga, ka, qda, kga), (qb, fb, gb, kb, qdb, kgb))
        ):
            at = h * width + g * ka
            spike = bias[:, 2 * h + g : 2 * h + g + 1]
            total, state = prepare(q_ref, f_ref, g_ref, spike, k, h, qd, kg, at)
            high = total.astype(jnp.bfloat16)
            low = (total - high.astype(jnp.float32)).astype(jnp.bfloat16)
            msg[:dv, at : at + k] = state[g * dv : (g + 1) * dv].astype(jnp.bfloat16)
            first = lax.broadcasted_iota(jnp.int32, (16, k), 0) == 0
            msg[dv:, at : at + k] = jnp.where(first, high, low)

    pl.semaphore_wait(barrier, n_sp - 1)

    def copy_to(k):
        return pltpu.make_async_remote_copy(
            src_ref=msg, dst_ref=inbox.at[place], send_sem=send_sem.at[k],
            recv_sem=recv_sem.at[place], device_id={"sp": lax.rem(place + k, n_sp)},
            device_id_type=MESH_ID,
        )

    for k in range(1, n_sp):
        @pl.when(place + k < n_sp)
        def _():
            copy_to(k).start()

    lane = lax.broadcasted_iota(jnp.int32, (rows, pair), 1)

    def scored(qd, kg, v):
        scores = lax.dot_general(qd, kg, NT, preferred_element_type=jnp.float32)
        scores = jnp.where(causal, scores, 0.0).astype(jnp.bfloat16)
        return jnp.dot(scores, v, preferred_element_type=jnp.float32)

    for h in range(heads):
        v = val[:, h * pair : (h + 1) * pair]
        out_a = scored(qda[:, h * ka : (h + 1) * ka], kga[:, h * ka : (h + 1) * ka], v)
        out_b = scored(qdb[:, h * kb : (h + 1) * kb], kgb[:, h * kb : (h + 1) * kb], v)
        raw[:, h * pair : (h + 1) * pair] = jnp.where(lane < dv, out_a, out_b)

    carry[...] = jnp.zeros_like(carry)
    for j in range(n_sp - 1):
        @pl.when(j < place)
        def _():
            pltpu.make_async_remote_copy(
                src_ref=msg, dst_ref=inbox.at[j], send_sem=send_sem.at[0],
                recv_sem=recv_sem.at[j], device_id={"sp": place}, device_id_type=MESH_ID,
            ).wait_recv()
            total = inbox[j, dv : dv + 1, :].astype(jnp.float32) + inbox[
                j, dv + 1 : dv + 2, :
            ].astype(jnp.float32)
            carry[...] = jnp.exp(total) * carry[...] + inbox[j, :dv, :].astype(jnp.float32)

    gains = jnp.concatenate([gain[...], gain[...]], axis=1)
    for h in range(heads):
        c = carry[:, h * width : (h + 1) * width].astype(jnp.bfloat16)
        zero_a = jnp.zeros((dv, ka), jnp.bfloat16)
        zero_b = jnp.zeros((dv, kb), jnp.bfloat16)
        state_a = jnp.concatenate([c[:, :ka], zero_a], axis=0)
        state_b = jnp.concatenate([zero_b, c[:, ka:]], axis=0)
        cols = slice(h * pair, (h + 1) * pair)
        x = raw[:, cols]
        x = x + lax.dot_general(
            qda[:, h * ka : (h + 1) * ka], state_a, NT, preferred_element_type=jnp.float32
        )
        x = x + lax.dot_general(
            qdb[:, h * kb : (h + 1) * kb], state_b, NT, preferred_element_type=jnp.float32
        )
        squares = x * x
        sum_a = jnp.sum(jnp.where(lane < dv, squares, 0.0), axis=1, keepdims=True)
        sum_b = jnp.sum(jnp.where(lane < dv, 0.0, squares), axis=1, keepdims=True)
        scale = lax.rsqrt(jnp.where(lane < dv, sum_a, sum_b) * (1.0 / dv) + EPSILON)
        open_gate = 1.0 / (1.0 + jnp.exp(-gate[:, cols].astype(jnp.float32)))
        out[:, cols] = (x * scale * gains * open_gate).astype(jnp.bfloat16)

    for k in range(1, n_sp):
        @pl.when(place + k < n_sp)
        def _():
            copy_to(k).wait_send()


def mixer(qa, fa, ga, qb, fb, gb, val, gate, bias, gain):
    n_sp = lax.axis_size("sp")
    rows = qa.shape[0]
    heads = bias.shape[1] // 2
    ka, kb = qa.shape[1] // heads, qb.shape[1] // heads
    dv = gain.shape[0]
    width = ka + kb
    bf, f32 = jnp.bfloat16, jnp.float32
    vm = pl.BlockSpec(memory_space=pltpu.VMEM)
    return pl.pallas_call(
        functools.partial(mixer_kernel, n_sp, heads, ka, kb, dv),
        out_shape=jax.ShapeDtypeStruct(val.shape, bf),
        in_specs=[vm] * 10,
        out_specs=vm,
        scratch_shapes=[
            pltpu.VMEM((dv + 16, heads * width), bf),
            pltpu.VMEM((n_sp, dv + 16, heads * width), bf),
            pltpu.VMEM((dv, heads * width), f32),
            pltpu.VMEM(qa.shape, bf),
            pltpu.VMEM(qb.shape, bf),
            pltpu.VMEM(qa.shape, bf),
            pltpu.VMEM(qb.shape, bf),
            pltpu.VMEM(val.shape, f32),
            pltpu.SemaphoreType.DMA((n_sp,)),
            pltpu.SemaphoreType.DMA((n_sp,)),
        ],
        compiler_params=pltpu.CompilerParams(
            collective_id=0, has_side_effects=True, vmem_limit_bytes=48 << 20
        ),
        name="mixer",
    )(qa, fa, ga.reshape(1, -1), qb, fb, gb.reshape(1, -1), val, gate, bias, gain.reshape(1, -1))


def landed(ref, sem, source):
    pltpu.make_async_remote_copy(
        src_ref=ref, dst_ref=ref, send_sem=sem, recv_sem=sem, device_id=source,
        device_id_type=MESH_ID,
    ).wait_recv()


def line_reduce(z, core, nz, rows, part, twin, box_r, box_l, out_r, out_l, sems, to_right, to_left, eager):
    twin_recv, send_r, recv_r, send_l, recv_l = sems
    chunks = part.shape[1]
    own = pl.ds(pl.multiple_of(core * rows, rows), rows)

    def base(d, ch):
        return part[d, ch, own, :].astype(jnp.float32) + twin[d, ch].astype(jnp.float32)

    def twin_wait(d):
        landed(twin.at[d], twin_recv.at[d], to_right)

    def hop(out, box, send, recv, d, ch, to):
        return pltpu.make_async_remote_copy(
            src_ref=out.at[d, ch], dst_ref=box.at[d, ch], send_sem=send.at[d, ch],
            recv_sem=recv.at[d, ch], device_id=to, device_id_type=MESH_ID,
        )

    def side(d, has_in, out, box, send, recv, to):
        twin_wait(d)
        for ch in range(chunks):
            @pl.when(has_in)
            def _():
                hop(out, box, send, recv, d, ch, to).wait_recv()
                total = base(d, ch) + box[d, ch].astype(jnp.float32)
                out[d, ch] = total.astype(jnp.bfloat16)

            @pl.when(jnp.logical_not(has_in))
            def _():
                out[d, ch] = base(d, ch).astype(jnp.bfloat16)

            hop(out, box, send, recv, d, ch, to).start()

    def right(d):
        side(d, z > 0, out_r, box_r, send_r, recv_r, to_right)

    def left(d):
        side(d, z < nz - 1, out_l, box_l, send_l, recv_l, to_left)

    def far_first(tau, _):
        @pl.when((tau >= z) & (z < nz - 1))
        def _():
            right(nz - 1 + z - tau)

        @pl.when((tau + z >= nz - 1) & (z > 0))
        def _():
            left(tau + z - (nz - 1))

        return 0

    def near_first(k, _):
        d = nz - 1 - k
        lefts = (d < z) & (z < nz - 1)

        @pl.when(lefts & (z >= nz // 2))
        def _():
            left(d)

        @pl.when((k > z) & (z > 0))
        def _():
            right(k)

        @pl.when(lefts & (z < nz // 2))
        def _():
            left(d)

        return 0

    def run():
        if eager:
            lax.fori_loop(1, nz, near_first, 0)
        else:
            lax.fori_loop(0, nz - 1, far_first, 0)

    def edge(d):
        @pl.when((z == 0) & (d > 0))
        def _():
            right(d)

        @pl.when((z == nz - 1) & (d < nz - 1))
        def _():
            left(d)

    def finish(total):
        twin_wait(z)
        for ch in range(chunks):
            total[ch] = base(z, ch)

            @pl.when(z > 0)
            def _():
                hop(out_r, box_r, send_r, recv_r, z, ch, to_right).wait_recv()
                total[ch] = total[ch] + box_r[z, ch].astype(jnp.float32)

            @pl.when(z < nz - 1)
            def _():
                hop(out_l, box_l, send_l, recv_l, z, ch, to_left).wait_recv()
                total[ch] = total[ch] + box_l[z, ch].astype(jnp.float32)

    def drain():
        def one(d, _):
            for ch in range(chunks):
                @pl.when(d > z)
                def _():
                    hop(out_r, box_r, send_r, recv_r, d, ch, to_right).wait_send()

                @pl.when(d < z)
                def _():
                    hop(out_l, box_l, send_l, recv_l, d, ch, to_left).wait_send()

            return 0

        lax.fori_loop(0, nz, one, 0)

    return run, edge, finish, drain


def experts_kernel(
    dv, n_sp, nz, cap, fold, pad,
    heads, alpha, beta, skip, gain1, gain2, gain3, router, w1, w2, w3, cluster,
    out,
    wcat, w1v, w2v, w3v, part, twin, box_r, box_l, out_r, out_l, mixed, hmid, placing,
    sp_out, sp_in, xs, part2, twin2, box_r2, box_l2, out_r2, out_l2, summed, back_out, back_in,
    wsem, tw_s, tw_r, rs_sr, rs_rr, rs_sl, rs_rl, sp_s, sp_r,
    ag_sr, ag_rr, ag_sl, ag_rl, ag_ds, ag_dr,
    tw2_s, tw2_r, rs2_sr, rs2_rr, rs2_sl, rs2_rl, bk_s, bk_r,
):
    f32, bf = jnp.float32, jnp.bfloat16
    place, t = lax.axis_index("sp"), lax.axis_index("tp")
    z, core = t // 2, t % 2
    peer = {"tp": z * 2 + 1 - core}
    to_right = {"tp": jnp.minimum(z + 1, nz - 1) * 2 + core}
    to_left = {"tp": jnp.maximum(z - 1, 0) * 2 + core}

    barrier = pltpu.get_barrier_semaphore()
    for k in range(1, n_sp):
        pl.semaphore_signal(
            barrier, inc=1, device_id={"sp": lax.rem(place + k, n_sp)}, device_id_type=MESH_ID
        )
    pl.semaphore_signal(barrier, inc=1, device_id=peer, device_id_type=MESH_ID)

    @pl.when(z < nz - 1)
    def _():
        pl.semaphore_signal(barrier, inc=1, device_id=to_right, device_id_type=MESH_ID)

    @pl.when(z > 0)
    def _():
        pl.semaphore_signal(barrier, inc=1, device_id=to_left, device_id_type=MESH_ID)

    loads = [
        pltpu.make_async_copy(src.at[0], dst, wsem.at[i])
        for i, (src, dst) in enumerate(((w1, w1v), (w2, w2v), (w3, w3v)))
    ]
    for load in loads:
        load.start()

    rows, width = skip.shape
    chunks = part.shape[1]
    half = width // chunks
    slots = n_sp * pad
    compact = xs.shape[2] // 2
    for h in range(alpha.shape[0] // dv):
        wcat[2 * h * dv : (2 * h + 1) * dv] = alpha[h * dv : (h + 1) * dv]
        wcat[(2 * h + 1) * dv : (2 * h + 2) * dv] = beta[h * dv : (h + 1) * dv]

    pl.semaphore_wait(
        barrier,
        n_sp + jnp.where(z > 0, 1, 0) + jnp.where(z < nz - 1, 1, 0),
    )

    def twin_copy(src, dst, d, size, send, recv):
        theirs = pl.ds(pl.multiple_of((1 - core) * size, size), size)
        return pltpu.make_async_remote_copy(
            src_ref=src.at[d, :, theirs, :], dst_ref=dst.at[d], send_sem=send.at[d],
            recv_sem=recv.at[d], device_id=peer, device_id_type=MESH_ID,
        )

    def project(i, _):
        d = jnp.where(i % 2 == 0, nz - 1 - i // 2, i // 2)
        x = heads[pl.ds(pl.multiple_of(d * 2 * rows, 2 * rows), 2 * rows), :]
        for ch in range(chunks):
            part[d, ch] = jnp.dot(
                x, wcat[:, ch * half : (ch + 1) * half], preferred_element_type=f32
            ).astype(bf)
        twin_copy(part, twin, d, rows, tw_s, tw_r).start()
        return 0

    lax.fori_loop(0, nz, project, 0)
    run, _, finish, drain = line_reduce(
        z, core, nz, rows, part, twin, box_r, box_l, out_r, out_l,
        (tw_r, rs_sr, rs_rr, rs_sl, rs_rl), to_right, to_left, False,
    )
    run()
    finish(mixed)

    def whole(ref):
        return jnp.concatenate([ref[ch] for ch in range(chunks)], axis=1)

    mid = skip[...].astype(f32) + rms_scale(whole(mixed), gain1[...])
    hmid[...] = mid.astype(bf)
    normed = rms_scale(hmid[...].astype(f32), gain2[...]).astype(bf)

    group = cluster[...]
    onehot = lax.broadcasted_iota(jnp.int32, (n_sp, rows), 0) == group
    ones = jnp.where(onehot, 1.0, 0.0)
    upto = jnp.where(
        lax.broadcasted_iota(jnp.int32, (rows, rows), 0)
        <= lax.broadcasted_iota(jnp.int32, (rows, rows), 1),
        1.0,
        0.0,
    ).astype(bf)
    counts = jnp.dot(ones.astype(bf), upto, preferred_element_type=f32)
    rank = jnp.sum(ones * counts, axis=0, keepdims=True).astype(jnp.int32) - 1
    slot = group * pad + rank * fold
    slot_id = lax.broadcasted_iota(jnp.int32, (slots, rows), 0)
    for q in range(fold):
        placing[q] = jnp.where(slot_id == slot + q, 1.0, 0.0).astype(bf)
    line_id = lax.broadcasted_iota(jnp.int32, (compact, 1), 0)
    source = jnp.zeros((compact, 1), jnp.int32)
    for j in range(1, n_sp):
        source = source + jnp.where(line_id >= j * cap, 1, 0)
    first = source * pad + (line_id - source * cap) * fold
    first = jnp.where(line_id < n_sp * cap, first, -fold)
    column = lax.broadcasted_iota(jnp.int32, (compact, slots), 1)
    packing = [jnp.where(column == first + q, 1.0, 0.0).astype(bf) for q in range(fold)]

    def sp_copy(src, dst, k, send, recv):
        g = lax.rem(place + k, n_sp)
        return pltpu.make_async_remote_copy(
            src_ref=src.at[g], dst_ref=dst.at[place], send_sem=send.at[g],
            recv_sem=recv.at[place], device_id={"sp": g}, device_id_type=MESH_ID,
        )

    def sp_exchange(src, dst, send, recv):
        for k in range(1, n_sp):
            sp_copy(src, dst, k, send, recv).start()
        dst[place] = src[place]
        for k in range(1, n_sp):
            g = lax.rem(place + k, n_sp)
            landed(dst.at[g], recv.at[g], peer)

    piece = width // fold

    def cut(x, q):
        return x[:, q * piece : (q + 1) * piece]

    placed = 0.0
    for q in range(fold):
        placed = placed + jnp.dot(placing[q], cut(normed, q), preferred_element_type=f32)
    sp_out[...] = placed.astype(bf).reshape(n_sp, pad, piece)
    sp_exchange(sp_out, sp_in, sp_s, sp_r)
    arrived = sp_in[...].reshape(slots, piece)
    packed = jnp.concatenate(
        [
            jnp.dot(packing[q], arrived, preferred_element_type=f32).astype(bf)
            for q in range(fold)
        ],
        axis=1,
    )
    mine = pl.ds(pl.multiple_of(core * compact, compact), compact)
    theirs = pl.ds(pl.multiple_of((1 - core) * compact, compact), compact)
    for ch in range(chunks):
        xs[z, ch, mine, :] = packed[:, ch * half : (ch + 1) * half]

    for load in loads:
        load.wait()

    def spread(d, ch, send, recv, to):
        return pltpu.make_async_remote_copy(
            src_ref=xs.at[d, ch, mine, :], dst_ref=xs.at[d, ch, mine, :],
            send_sem=send.at[d, ch], recv_sem=recv.at[d, ch], device_id=to,
            device_id_type=MESH_ID,
        )

    member = t * w1v.shape[1] // FF

    def expert(d):
        for ch in range(chunks):
            landed(xs.at[d, ch, theirs, :], ag_dr.at[d, ch], peer)
        gate = up = score = 0.0
        for ch in range(chunks):
            x = xs[d, ch]
            depth = pl.ds(ch * half, half)
            gate = gate + jnp.dot(x, w1v[depth, :], preferred_element_type=f32)
            up = up + jnp.dot(x, w2v[depth, :], preferred_element_type=f32)
            score = score + jnp.dot(x, router[depth, :], preferred_element_type=f32)
        score = 1.0 / (1.0 + jnp.exp(-score))
        picked = lax.broadcasted_iota(jnp.int32, score.shape, 1) == member
        weight = jnp.sum(jnp.where(picked, score, 0.0), axis=1, keepdims=True) / jnp.sum(
            score, axis=1, keepdims=True
        )
        hidden = (gate / (1.0 + jnp.exp(-gate)) * up).astype(bf)
        for ch in range(chunks):
            y = jnp.dot(hidden, w3v[:, ch * half : (ch + 1) * half], preferred_element_type=f32)
            part2[d, ch] = (weight * y).astype(bf)
        twin_copy(part2, twin2, d, compact, tw2_s, tw2_r).start()

    run2, edge2, finish2, drain2 = line_reduce(
        z, core, nz, compact, part2, twin2, box_r2, box_l2, out_r2, out_l2,
        (tw2_r, rs2_sr, rs2_rr, rs2_sl, rs2_rl), to_right, to_left, True,
    )

    def gather(tau, _):
        low, high = z - tau, z + tau
        for ch in range(chunks):
            @pl.when(low >= 0)
            def _():
                @pl.when(tau > 0)
                def _():
                    spread(low, ch, ag_sr, ag_rr, to_right).wait_recv()

                @pl.when(z < nz - 1)
                def _():
                    spread(low, ch, ag_sr, ag_rr, to_right).start()

                spread(low, ch, ag_ds, ag_dr, peer).start()

            @pl.when(high < nz)
            def _():
                @pl.when(tau > 0)
                def _():
                    spread(high, ch, ag_sl, ag_rl, to_left).wait_recv()

                @pl.when(z > 0)
                def _():
                    spread(high, ch, ag_sl, ag_rl, to_left).start()

                @pl.when(tau > 0)
                def _():
                    spread(high, ch, ag_ds, ag_dr, peer).start()

        @pl.when(low >= 0)
        def _():
            expert(low)
            edge2(low)

        @pl.when((high < nz) & (tau > 0))
        def _():
            expert(high)
            edge2(high)

        return 0

    lax.fori_loop(0, nz, gather, 0)
    run2()
    finish2(summed)
    total = whole(summed).astype(bf)
    placed = 0.0
    for q in range(fold):
        placed = placed + lax.dot_general(
            packing[q], cut(total, q), TN, preferred_element_type=f32
        )
    back_out[...] = placed.astype(bf).reshape(n_sp, pad, piece)
    sp_exchange(back_out, back_in, bk_s, bk_r)
    arrived = back_in[...].reshape(slots, piece)
    routed = jnp.concatenate(
        [
            lax.dot_general(placing[q], arrived, TN, preferred_element_type=f32)
            for q in range(fold)
        ],
        axis=1,
    )
    out[...] = (hmid[...].astype(f32) + rms_scale(routed, gain3[...])).astype(bf)

    drain()
    drain2()

    def settle(d, _):
        twin_copy(part, twin, d, rows, tw_s, tw_r).wait_send()
        twin_copy(part2, twin2, d, compact, tw2_s, tw2_r).wait_send()
        for ch in range(chunks):
            spread(d, ch, ag_ds, ag_dr, peer).wait_send()

            @pl.when((d <= z) & (z < nz - 1))
            def _():
                spread(d, ch, ag_sr, ag_rr, to_right).wait_send()

            @pl.when((d >= z) & (z > 0))
            def _():
                spread(d, ch, ag_sl, ag_rl, to_left).wait_send()

        return 0

    lax.fori_loop(0, nz, settle, 0)
    for k in range(1, n_sp):
        sp_copy(sp_out, sp_in, k, sp_s, sp_r).wait_send()
        sp_copy(back_out, back_in, k, bk_s, bk_r).wait_send()


def mixture(dv, heads, alpha, beta, skip, g1, g2, g3, router, w1, w2, w3, cluster):
    n_sp, nz = lax.axis_size("sp"), lax.axis_size("tp") // 2
    rows, width = skip.shape
    cap = (9 * rows + 8 * n_sp - 1) // (8 * n_sp)
    fold = 4
    pad = (cap * fold + 15) // 16 * 16
    compact = (n_sp * cap + 15) // 16 * 16
    chunks = CHUNKS
    half = width // chunks
    f32, bf = jnp.float32, jnp.bfloat16
    vm = pl.BlockSpec(memory_space=pltpu.VMEM)
    hbm = pl.BlockSpec(memory_space=pl.ANY)
    line = (nz, chunks, rows, half)
    line2 = (nz, chunks, compact, half)
    dma = pltpu.SemaphoreType.DMA
    reduce_sems = [dma((nz,))] * 2 + [dma((nz, chunks))] * 4
    return pl.pallas_call(
        functools.partial(experts_kernel, dv, n_sp, nz, cap, fold, pad),
        out_shape=jax.ShapeDtypeStruct(skip.shape, bf),
        in_specs=[vm] * 8 + [hbm] * 3 + [vm],
        out_specs=vm,
        scratch_shapes=[
            pltpu.VMEM((2 * alpha.shape[0], width), bf),
            pltpu.VMEM(w1.shape[1:], bf),
            pltpu.VMEM(w2.shape[1:], bf),
            pltpu.VMEM(w3.shape[1:], bf),
            pltpu.VMEM((nz, chunks, 2 * rows, half), bf),
        ]
        + [pltpu.VMEM(line, bf)] * 5
        + [
            pltpu.VMEM(line[1:], f32),
            pltpu.VMEM(skip.shape, bf),
            pltpu.VMEM((fold, n_sp * pad, rows), bf),
            pltpu.VMEM((n_sp, pad, width // fold), bf),
            pltpu.VMEM((n_sp, pad, width // fold), bf),
            pltpu.VMEM((nz, chunks, 2 * compact, half), bf),
            pltpu.VMEM((nz, chunks, 2 * compact, half), bf),
        ]
        + [pltpu.VMEM(line2, bf)] * 5
        + [
            pltpu.VMEM(line2[1:], f32),
            pltpu.VMEM((n_sp, pad, width // fold), bf),
            pltpu.VMEM((n_sp, pad, width // fold), bf),
            dma((3,)),
        ]
        + reduce_sems
        + [dma((n_sp,))] * 2
        + [dma((nz, chunks))] * 6
        + reduce_sems
        + [dma((n_sp,))] * 2,
        compiler_params=pltpu.CompilerParams(
            collective_id=1, has_side_effects=True, vmem_limit_bytes=60 << 20
        ),
        name="mixture",
    )(
        heads, alpha, beta, skip, g1.reshape(1, -1), g2.reshape(1, -1), g3.reshape(1, -1),
        router, w1, w2, w3, cluster.reshape(1, -1),
    )


def shards(
    ask_preactivation_left,
    keep_preactivation_left,
    keep_bound_complement_left,
    ask_preactivation_right,
    keep_preactivation_right,
    keep_bound_complement_right,
    payload_entries,
    emission_switch_logits,
    added_log_keep_bias,
    lanewise_rescale,
    emission_matrix_alpha,
    emission_matrix_beta,
    skip_stream,
    postrecurrence_rescale,
    premixture_rescale,
    postmixture_rescale,
    dispatcher_columns,
    switch_matrix,
    expansion_matrix,
    contraction_matrix,
    item_specialist_cluster,
):
    heads = mixer(
        ask_preactivation_left,
        keep_preactivation_left,
        keep_bound_complement_left,
        ask_preactivation_right,
        keep_preactivation_right,
        keep_bound_complement_right,
        payload_entries,
        emission_switch_logits,
        added_log_keep_bias,
        lanewise_rescale,
    )
    return mixture(
        lanewise_rescale.shape[0],
        heads,
        emission_matrix_alpha,
        emission_matrix_beta,
        skip_stream,
        postrecurrence_rescale,
        premixture_rescale,
        postmixture_rescale,
        dispatcher_columns,
        switch_matrix,
        expansion_matrix,
        contraction_matrix,
        item_specialist_cluster,
    )


def solution(mesh):
    placed = (
        P("sp", "tp"),
        P("sp", "tp"),
        P("tp"),
        P("sp", "tp"),
        P("sp", "tp"),
        P("tp"),
        P("sp", "tp"),
        P("sp", "tp"),
        P("sp", "tp"),
        P(),
        P("tp", None),
        P("tp", None),
        P(("sp", "tp"), None),
        P(),
        P(),
        P(),
        P(None, "sp"),
        P("sp", None, "tp"),
        P("sp", None, "tp"),
        P("sp", "tp", None),
        P(("sp", "tp")),
    )
    return jax.shard_map(
        shards, mesh=mesh, in_specs=placed, out_specs=P(("sp", "tp"), None), check_vma=False
    )
```
